512 devices in a mesh: grp: 2 (over y), sp: 16 (over z), dp: 16 (over x, core).
Axes of the slice: x: 8, y: 2, z: 16, core: 2. Of those that a mesh axis runs over, the one named last changes fastest.
The devices are a block of a 8x8x16 slice.
Arguments:
- queries: bfloat16 [32, 2048, 16, 192], P(('grp', 'dp'), 'sp'), parts along dimension 0, may hold values from -41 to 41
- kv_latent: bfloat16 [32, 2048, 512], P(('grp', 'dp'), 'sp'), parts along dimension 0, may hold values from -6 to 6
- rope_key: bfloat16 [32, 2048, 64], P(('grp', 'dp'), 'sp'), parts along dimension 0, may hold values from -5.1 to 5.1
- kv_gain: float32 [512], replicated, may hold values from 0.1 to 1.9
- kv_weight: bfloat16 [512, 4096], P('dp', 'sp'), may hold values from -0.25 to 0.25
- out_weight: bfloat16 [2048, 2048], P(None, 'dp'), may hold values from -1 to 1
Outputs:
- mixed: bfloat16 [32, 2048, 2048], P(('grp', 'dp'), 'sp'), parts along dimension 0
The draws below stay inside these ranges and needn't reach their ends.
There are 2 independent parts, one for each index of `grp`. The reference program is written for one: setup_inputs(seed, part) draws one part's arguments, and reference() takes and returns one part's arrays. A program takes and returns all parts, laid end to end along the dimension named above; an argument that names none is the same for every part. Nothing has to cross between parts.
All inputs are finite; a program needn't handle non-finite values.
Results may differ from the reference program's by a relative error of at most 0.0075.
Values may be sent and summed in bfloat16 or wider, within the bound.
A program may use at most 64 MiB of HBM per device.

```python
import jax
import jax.numpy as jnp
from jax import lax

D = 2048
H = 16
KL = 512
NOPE = 128
ROPE = 64
VD = 128
LEN = 2048
SEQS = 16


def paired_draw(key):
    base = jax.random.fold_in(key, 41)
    first_key, second_key = jax.random.split(base)
    query_shape = (SEQS, LEN, H, NOPE + ROPE)
    shared = jnp.clip(jax.random.normal(first_key, (SEQS, LEN, ROPE), jnp.float32), -5.0, 5.0)
    query = jnp.clip(jax.random.normal(second_key, query_shape, jnp.float32), -5.0, 5.0)
    return (query, shared)


def draw_queries(key, part):
    return paired_draw(key)[0].astype(jnp.bfloat16)


def draw_rope_key(key, part):
    return paired_draw(key)[1].astype(jnp.bfloat16)


def levels(stream_key, shape, cuts, smallest, high):
    level, own = 1.0, jax.random.fold_in(stream_key, 6)
    for position, parts in cuts:
        draws = jnp.exp(jax.random.uniform(jax.random.fold_in(own, position), (parts,), jnp.float32, smallest / len(cuts), high / len(cuts)))
        level = level * jnp.repeat(draws, shape[position] // parts).reshape([-1 if axis == position else 1 for axis in range(len(shape))])
    return level


def scatter_about(own_key, shape, scale, bound, cuts=(), kind=jnp.bfloat16):
    gain = levels(own_key, shape, cuts, -0.22, 0.18) if cuts else 1.0
    values = jax.random.normal(own_key, shape, jnp.float32) * scale * gain
    return jnp.minimum(jnp.maximum(values, -bound), bound).astype(kind)


def setup_inputs(seed: int = 0, part: int = 0) -> dict:
    seeds = jax.random.split(jax.random.key(seed), 7)
    part_splits = jax.random.split(jax.random.fold_in(seeds[6], part), 7)
    return {
        "queries": draw_queries(jax.random.fold_in(jax.random.fold_in(seeds[6], part), 71), part),
        "kv_latent": scatter_about(part_splits[1], (SEQS, LEN, KL), 1.0, 6.0, ((0, 16), (1, 16))),
        "rope_key": draw_rope_key(jax.random.fold_in(jax.random.fold_in(seeds[6], part), 71), part),
        "kv_gain": jnp.clip(1.0 + 0.18 * jax.random.normal(seeds[3], (KL,), jnp.float32), 0.1, 1.9),
        "kv_weight": scatter_about(seeds[4], (KL, H * (NOPE + VD)), KL ** -0.5, 0.25, ((0, 16), (1, 16))),
        "out_weight": scatter_about(seeds[5], (H * VD, D), 32 ** -0.5, 1.0, ((1, 16),)),
    }


def rotate(values, positions):
    half = values.shape[-1] // 2
    inverse = jnp.power(10000.0, -jnp.arange(half, dtype=jnp.float32) * 2.0 / values.shape[-1])
    angle = positions.astype(jnp.float32)[..., None] * inverse
    first = values[..., :half].astype(jnp.float32)
    second = values[..., half:].astype(jnp.float32)
    cosine = jnp.cos(angle)
    sine = jnp.sin(angle)
    return jnp.concatenate([first * cosine - second * sine, first * sine + second * cosine], axis=-1)

def attend(query_rot, key_value, key_rot):
    length, heads = (query_rot.shape[0], query_rot.shape[1])
    nope = query_rot.shape[2] - key_rot.shape[1]
    scale = query_rot.shape[2] ** (-0.5)
    content = key_value[:, :, :nope]
    values = key_value[:, :, nope:].astype(jnp.float32)
    shared = jnp.broadcast_to(key_rot[:, None, :], (length, heads, key_rot.shape[1]))
    keys = jnp.concatenate([content, shared], axis=-1).astype(jnp.float32)
    block = min(512, length)
    blocks = query_rot.reshape(length // block, block, heads, query_rot.shape[2])
    key_pos = jnp.arange(length, dtype=jnp.int32)

    def one_block(item):
        query_block, index = item
        scores = jnp.einsum('qhd,khd->hqk', query_block.astype(jnp.float32), keys) * scale
        query_pos = index * block + jnp.arange(block, dtype=jnp.int32)
        kept = query_pos[:, None] >= key_pos[None, :]
        scores = jnp.where(kept[None], scores, -jnp.inf)
        top = lax.optimization_barrier(jnp.max(scores, axis=-1, keepdims=True))
        expo = jnp.exp(scores - top)
        probs = (expo / lax.optimization_barrier(jnp.sum(expo, axis=-1, keepdims=True))).astype(jnp.bfloat16)
        return jnp.einsum('hqk,khd->qhd', probs.astype(jnp.float32), values).astype(jnp.bfloat16)
    result = lax.map(one_block, (blocks, jnp.arange(length // block, dtype=jnp.int32)))
    return result.reshape(length, heads, values.shape[2])

def reference(queries, kv_latent, rope_key, kv_gain, kv_weight, out_weight):
    positions = jnp.arange(LEN, dtype=jnp.int32)

    def one_sequence(item):
        query, latent, shared = item
        latent32 = latent.astype(jnp.float32)
        latent_n = (latent32 * lax.rsqrt(lax.optimization_barrier(jnp.mean(latent32 * latent32, axis=-1, keepdims=True)) + 1e-06) * kv_gain).astype(jnp.bfloat16)
        key_value = jnp.dot(latent_n, kv_weight, preferred_element_type=jnp.float32).astype(jnp.bfloat16)
        key_value = key_value.reshape(LEN, H, NOPE + VD)
        key_rot = rotate(shared, positions).astype(jnp.bfloat16)
        turned = rotate(query[:, :, NOPE:], positions[:, None])
        query_rot = jnp.concatenate([query[:, :, :NOPE].astype(jnp.float32), turned], axis=-1).astype(jnp.bfloat16)
        attended = attend(query_rot, key_value, key_rot).reshape(LEN, H * VD)
        return jnp.dot(attended, out_weight, preferred_element_type=jnp.float32).astype(jnp.bfloat16)
    return lax.map(one_sequence, (queries, kv_latent, rope_key))
```

```python
import functools
import math

import jax
import jax.numpy as jnp
import numpy as np
from jax import lax
from jax.experimental import pallas as pl
from jax.experimental.pallas import tpu as pltpu
from jax.sharding import PartitionSpec as P

NOPE = 128
VD = 128
MESH = pl.DeviceIdType.MESH
F32 = jnp.float32
BF16 = jnp.bfloat16
FWD, BWD = 0, 1
LCH = 4
OCH = 8
XPRE = 16
NEG = -1e30


def when(cond, fn):
    if isinstance(cond, (bool, np.bool_)):
        if cond:
            fn()
    else:
        pl.when(cond)(fn)


def kernel(
    nz, ndp,
    q_hbm, lat_hbm, rope_hbm, gain_hbm, wkv_hbm, wout_hbm, cos_hbm, sin_hbm,
    out_hbm,
    lbuf, rbuf, wkv, wout, qraw, qbuf, kbuf, vbuf, sbuf, att, obuf,
    lat, rope, gain, cosv, sinv,
    load_sem, zl_recv, zw_recv, x_recv, xw_recv, dw_recv, do_recv,
    zl_send, zl8_send, zr_send, zw_send, zw8_send, x_send, x4_send, xw_send, dw_send, do_send,
    out_sem,
):
    nx = ndp // 2
    hz, hx = nz // 2, nx // 2
    tok = lat.shape[0]
    kl = lat.shape[1]
    z = lax.axis_index("sp")
    dp = lax.axis_index("dp")
    x = dp // 2
    c = dp % 2
    o = 1 - c
    zdev = [{"sp": (z + 1) % nz}, {"sp": (z + nz - 1) % nz}]
    xdev = [{"dp": (dp + 2) % ndp}, {"dp": (dp + ndp - 2) % ndp}]
    mate = {"dp": x * 2 + o}

    def zsrc(d, s):
        return (z + nz - s) % nz if d == FWD else (z + s) % nz

    def xsrc(d, s):
        return (x + nx - s) % nx if d == FWD else (x + s) % nx

    loads = [
        pltpu.make_async_copy(lat_hbm.at[0], lat, load_sem.at[0]),
        pltpu.make_async_copy(gain_hbm, gain, load_sem.at[1]),
        pltpu.make_async_copy(rope_hbm.at[0], rope, load_sem.at[2]),
        pltpu.make_async_copy(cos_hbm.at[z], cosv, load_sem.at[3]),
        pltpu.make_async_copy(sin_hbm.at[z], sinv, load_sem.at[4]),
        pltpu.make_async_copy(wkv_hbm, wkv.at[z, x, c], load_sem.at[5]),
        pltpu.make_async_copy(wout_hbm, wout.at[c, x], load_sem.at[6]),
        pltpu.make_async_copy(q_hbm.at[0], qraw, load_sem.at[7]),
    ]
    for copy in loads:
        copy.start()

    barrier = pltpu.get_barrier_semaphore()
    peers = zdev + [mate] + [{"dp": (dp + 2 * k) % ndp} for k in range(1, nx)]
    for peer in peers:
        pl.semaphore_signal(barrier, inc=1, device_id=peer, device_id_type=MESH)

    for copy in loads[:5]:
        copy.wait()
    value = lat[...].astype(F32)
    norm = value * lax.rsqrt(jnp.mean(value * value, axis=-1, keepdims=True) + 1e-06)
    lbuf[z] = (norm * gain[...]).astype(BF16)
    half = rope.shape[0] // 2

    def rotated(first, second):
        first = first.astype(F32)
        second = second.astype(F32)
        cosine, sine = cosv[...], sinv[...]
        return first * cosine - second * sine, first * sine + second * cosine

    turned = rotated(rope[0:half, :], rope[half:, :])
    rbuf[z, 0:half, :] = turned[0].astype(BF16)
    rbuf[z, half:, :] = turned[1].astype(BF16)
    loads[5].wait()
    loads[6].wait()
    pl.semaphore_wait(barrier, len(peers))

    rows = tok // LCH
    xs = nx // LCH
    orow = wout.shape[2] // OCH

    def l_ref(b, ch):
        return rbuf.at[b] if ch == LCH else lbuf.at[b, pl.ds(ch * rows, rows)]

    def l_copy(d, s, ch, b):
        if ch == LCH:
            ssem = zr_send.at[d]
        else:
            ssem = zl_send.at[d] if s < hz else zl8_send.at[d]
        return pltpu.make_async_remote_copy(
            src_ref=l_ref(b, ch), dst_ref=l_ref(b, ch), send_sem=ssem,
            recv_sem=zl_recv.at[d, s - 1, ch], device_id=zdev[d], device_id_type=MESH)

    def l_has(d, s, ch):
        if s < hz:
            return True
        return (ch == LCH or ch < LCH // 2) if d == FWD else LCH // 2 <= ch < LCH

    def l_event(s, ch):
        for d in (FWD, BWD):
            if not l_has(d, s, ch):
                continue
            l_copy(d, s, ch, zsrc(d, s)).wait_recv()
            if s < hz and l_has(d, s + 1, ch):
                l_copy(d, s + 1, ch, zsrc(d, s)).start()

    def w_ref(h, ch, core):
        return wkv.at[h, pl.ds(ch * xs, xs), core]

    def w_copy(d, s, ch, h, last):
        return pltpu.make_async_remote_copy(
            src_ref=w_ref(h, ch, c), dst_ref=w_ref(h, ch, c),
            send_sem=zw8_send.at[d] if last else zw_send.at[d],
            recv_sem=zw_recv.at[d, s - 1, ch], device_id=zdev[d], device_id_type=MESH)

    def w_mate(h, ch):
        return pltpu.make_async_remote_copy(
            src_ref=w_ref(h, ch, c), dst_ref=w_ref(h, ch, c), send_sem=dw_send,
            recv_sem=dw_recv.at[h], device_id=mate, device_id_type=MESH)

    def w_event(e):
        s = e // 2 + 1
        part = e % 2
        for d in (FWD, BWD):
            mine = part == d
            h = zsrc(d, s)

            def arrive(d=d, s=s, h=h, part=part):
                for k in range(LCH // 2):
                    w_copy(d, s, part * (LCH // 2) + k, h, False).wait_recv()

            def forward(last, d=d, s=s, h=h, part=part):
                for k in range(LCH // 2):
                    w_copy(d, s + 1, part * (LCH // 2) + k, h, last).start()

            def across(h=h, part=part):
                for k in range(LCH // 2):
                    w_mate(h, part * (LCH // 2) + k).start()

            if isinstance(e, int):
                if s < hz or (s == hz and mine):
                    arrive()
                    if s < hz - 1:
                        forward(False)
                    elif s == hz - 1 and mine:
                        forward(True)
                    across()
            else:
                def body(arrive=arrive, forward=forward, across=across, s=s, mine=mine):
                    arrive()
                    pl.when(s < hz - 1)(lambda: forward(False))
                    pl.when((s == hz - 1) & mine)(lambda: forward(True))
                    across()

                pl.when((s < hz) | ((s == hz) & mine))(body)

    def o_ref(b, ch):
        return wout.at[c, b, pl.ds(ch * orow, orow)]

    def o_copy(d, s, ch, b, last):
        return pltpu.make_async_remote_copy(
            src_ref=o_ref(b, ch), dst_ref=o_ref(b, ch),
            send_sem=x4_send.at[d] if last else x_send.at[d],
            recv_sem=x_recv.at[d, s - 1, ch], device_id=xdev[d], device_id_type=MESH)

    def o_mate(b, ch):
        return pltpu.make_async_remote_copy(
            src_ref=o_ref(b, ch), dst_ref=o_ref(b, ch), send_sem=do_send,
            recv_sem=do_recv, device_id=mate, device_id_type=MESH)

    nev = OCH * (hx - 1) + OCH // 2

    def o_event(n):
        s = n // OCH + 1
        k = n % OCH
        for d in (FWD, BWD):
            b = xsrc(d, s)
            if isinstance(n, int):
                ch = k if s < hx else k + d * (OCH // 2)
                o_copy(d, s, ch, b, False).wait_recv()
                if s < hx - 1:
                    o_copy(d, s + 1, ch, b, False).start()
                elif s == hx - 1 and (k < OCH // 2) == (d == FWD):
                    o_copy(d, s + 1, ch, b, True).start()
                o_mate(b, ch).start()
            else:
                ch = jnp.where(s < hx, k, k + d * (OCH // 2))
                o_copy(d, s, ch, b, False).wait_recv()
                half_ok = (k < OCH // 2) if d == FWD else (k >= OCH // 2)

                def forward(d=d, s=s, ch=ch, b=b, last=False):
                    o_copy(d, s + 1, ch, b, last).start()

                pl.when(s < hx - 1)(forward)
                pl.when((s == hx - 1) & half_ok)(functools.partial(forward, last=True))
                o_mate(b, ch).start()

    def xw_copy(k, b):
        return pltpu.make_async_remote_copy(
            src_ref=wkv.at[z, b, c], dst_ref=wkv.at[z, b, c], send_sem=xw_send,
            recv_sem=xw_recv, device_id={"dp": (dp + 2 * k) % ndp}, device_id_type=MESH)

    for k in range(1, nx):
        xw_copy(k, x).start()
    for ch in range(LCH + 1):
        for d in (FWD, BWD):
            l_copy(d, 1, ch, z).start()
    for ch in range(OCH):
        for d in (FWD, BWD):
            o_copy(d, 1, ch, x, False).start()
    for ch in range(OCH):
        o_mate(x, ch).start()

    def all_of(ref, send_sem, recv_sem):
        return pltpu.make_async_remote_copy(
            src_ref=ref, dst_ref=ref, send_sem=send_sem, recv_sem=recv_sem,
            device_id=mate, device_id_type=MESH)

    loads[7].wait()

    def prepare_query(h):
        content = qraw[h, 0:NOPE, :].astype(F32)
        t0, t1 = rotated(qraw[h, NOPE:NOPE + half, :], qraw[h, NOPE + half:, :])
        pad = jnp.zeros((256 - NOPE - 2 * half, tok), F32)
        whole = jnp.concatenate([content, t0, t1, pad], axis=0)
        qbuf[h] = whole.T.astype(BF16)

    def prepare_key(b):
        key = rbuf[b].astype(F32)
        pad = jnp.zeros((128 - 2 * half, tok), F32)
        kbuf[b, :, NOPE:] = jnp.concatenate([key, pad], axis=0).T.astype(BF16)

    prepare_key(z)
    per = nz // hz
    done = 0
    for s in range(1, hz + 1):
        for ch in range(LCH + 1):
            l_event(s, ch)
            if ch % 2 == 1 and done < XPRE and s > 1:
                o_event(done)
                done += 1
        if s < hz:
            for d in (FWD, BWD):
                prepare_key(zsrc(d, s))
        else:
            prepare_key(zsrc(FWD, s))
        for j in range(per):
            prepare_query((s - 1) * per + j)
        if s == 4:
            all_of(wkv.at[z, pl.ds(0, nx - 1), c], xw_send, xw_recv).wait_recv()
            for ch in range(LCH):
                for d in (FWD, BWD):
                    w_copy(d, 1, ch, z, False).start()
            for ch in range(LCH):
                w_mate(z, ch).start()
    while done < XPRE:
        o_event(done)
        done += 1

    w_event(0)

    span = 4 * tok
    scale = float((2 * half + NOPE) ** -0.5 * math.log2(math.e))

    def one_head(i, carry):
        step = (i + 1) // 2
        h = lax.rem(jnp.where(i % 2 == 1, z + nz - step, z + step), nz)
        all_of(wkv.at[h, :, o], dw_send, dw_recv.at[h]).wait_recv()
        weights = wkv[h].reshape(kl, NOPE + VD)
        for t in range(nz // 4):
            block = lbuf[4 * t:4 * t + 4].reshape(span, kl)
            kv = jnp.dot(block, weights, preferred_element_type=F32).astype(BF16)
            kbuf[4 * t:4 * t + 4, :, 0:NOPE] = kv[:, :NOPE].reshape(4, tok, NOPE)
            vbuf[4 * t:4 * t + 4] = kv[:, NOPE:].reshape(4, tok, VD)
        w_event(i + 1)
        pl.when(i < nev - XPRE)(lambda: o_event(i + XPRE))
        query = qbuf[h]
        row = z * tok + lax.broadcasted_iota(jnp.int32, (tok, span), 0)
        col = lax.broadcasted_iota(jnp.int32, (tok, span), 1)
        top = jnp.full((tok, 128), NEG, F32)
        for t in range(nz // 4):
            keys = kbuf[4 * t:4 * t + 4].reshape(span, 256)
            sc = lax.dot_general(query, keys, (((1,), (1,)), ((), ())), preferred_element_type=F32)
            sc = jnp.where(col + t * span <= row, sc * scale, NEG)
            sbuf[:, t * span:(t + 1) * span] = sc
            for j in range(span // 128):
                top = jnp.maximum(top, sc[:, j * 128:(j + 1) * 128])
        peak = jnp.max(top, axis=-1, keepdims=True)
        total = jnp.zeros((tok, 128), F32)
        result = jnp.zeros((tok, VD), F32)
        for t in range(nz // 4):
            expo = jnp.exp2(sbuf[:, t * span:(t + 1) * span] - peak)
            for j in range(span // 128):
                total = total + expo[:, j * 128:(j + 1) * 128]
            vals = vbuf[4 * t:4 * t + 4].reshape(span, VD)
            result = result + jnp.dot(expo.astype(BF16), vals, preferred_element_type=F32)
        denom = jnp.sum(total, axis=-1, keepdims=True)
        att[h] = (result / denom).astype(BF16)
        return carry

    lax.fori_loop(0, nz, one_head, 0)

    all_of(wout.at[o], do_send, do_recv).wait_recv()
    attended = jnp.concatenate([att[h] for h in range(nz)], axis=1)

    def out_copy(b):
        return pltpu.make_async_copy(
            obuf.at[b], out_hbm.at[0, :, pl.ds(b * 256, 256)], out_sem.at[b])

    def project(b, carry):
        cols = jnp.concatenate([wout[0, b], wout[1, b]], axis=1)
        obuf[b] = jnp.dot(attended, cols, preferred_element_type=F32).astype(BF16)
        out_copy(b).start()
        return carry

    lax.fori_loop(0, nx, project, 0)

    all_of(wkv.at[0, pl.ds(0, nx - 1), 0], xw_send, xw_recv).wait_send()
    for d in (FWD, BWD):
        all_of(lbuf.at[pl.ds(0, hz - 1)], zl_send.at[d], xw_recv).wait_send()
        all_of(lbuf.at[0, pl.ds(0, tok // 2)], zl8_send.at[d], xw_recv).wait_send()
        all_of(rbuf.at[pl.ds(0, hz if d == FWD else hz - 1)], zr_send.at[d], xw_recv).wait_send()
        all_of(wkv.at[pl.ds(0, hz - 1), :, 0], zw_send.at[d], xw_recv).wait_send()
        all_of(wkv.at[0, pl.ds(0, nx // 2), 0], zw8_send.at[d], xw_recv).wait_send()
        all_of(wout.at[0, pl.ds(0, hx - 1)], x_send.at[d], xw_recv).wait_send()
        all_of(wout.at[0, 0, pl.ds(0, wout.shape[2] // 2)], x4_send.at[d], xw_recv).wait_send()
    all_of(wkv.at[:, :, 0], dw_send, xw_recv).wait_send()
    all_of(wout.at[0], do_send, xw_recv).wait_send()
    for b in range(nx):
        out_copy(b).wait()


def body(nz, ndp, queries, kv_latent, rope_key, kv_gain, kv_weight, out_weight):
    tok, heads, width = queries.shape[1:]
    kl = kv_latent.shape[2]
    rot = rope_key.shape[2]
    half = rot // 2
    nx = ndp // 2
    hz, hx = nz // 2, nx // 2
    model = out_weight.shape[1] * ndp
    pos = np.arange(nz * tok, dtype=np.float32)
    inverse = np.power(np.float32(10000.0), -np.arange(half, dtype=np.float32) * np.float32(2.0) / np.float32(rot))
    angle = (pos[:, None] * inverse.astype(np.float32)).astype(np.float32).astype(np.float64)
    table = lambda f: jnp.asarray(
        f(angle).astype(np.float32).reshape(nz, tok, half).transpose(0, 2, 1))
    dma = pltpu.SemaphoreType.DMA
    anyspec = pl.BlockSpec(memory_space=pl.ANY)
    call = pl.pallas_call(
        functools.partial(kernel, nz, ndp),
        out_shape=jax.ShapeDtypeStruct((1, tok, model), BF16),
        in_specs=[anyspec] * 8,
        out_specs=anyspec,
        scratch_shapes=[
            pltpu.VMEM((nz, tok, kl), BF16),
            pltpu.VMEM((nz, rot, tok), BF16),
            pltpu.VMEM((nz, nx, 2, kl // ndp, NOPE + VD), BF16),
            pltpu.VMEM((2, nx, heads * VD, model // ndp), BF16),
            pltpu.VMEM((heads, width, tok), BF16),
            pltpu.VMEM((heads, tok, 256), BF16),
            pltpu.VMEM((nz, tok, 256), BF16),
            pltpu.VMEM((nz, tok, VD), BF16),
            pltpu.VMEM((tok, nz * tok), F32),
            pltpu.VMEM((heads, tok, VD), BF16),
            pltpu.VMEM((nx, tok, 256), BF16),
            pltpu.VMEM((tok, kl), BF16),
            pltpu.VMEM((rot, tok), BF16),
            pltpu.VMEM((1, kl), F32),
            pltpu.VMEM((half, tok), F32),
            pltpu.VMEM((half, tok), F32),
            dma((8,)),
            dma((2, hz, LCH + 1)),
            dma((2, hz, LCH)),
            dma((2, hx, OCH)),
            dma, dma((nz,)), dma,
            dma((2,)), dma((2,)), dma((2,)), dma((2,)), dma((2,)), dma((2,)), dma((2,)),
            dma, dma, dma,
            dma((nx,)),
        ],
        compiler_params=pltpu.CompilerParams(
            collective_id=0, has_side_effects=True, vmem_limit_bytes=60 * 1024 * 1024),
    )
    return call(
        jnp.transpose(queries, (0, 2, 3, 1)), kv_latent, jnp.transpose(rope_key, (0, 2, 1)),
        kv_gain.reshape(1, kl), kv_weight, out_weight, table(np.cos), table(np.sin))


def solution(mesh):
    return jax.shard_map(
        functools.partial(body, mesh.shape["sp"], mesh.shape["dp"]),
        mesh=mesh,
        in_specs=(
            P(("grp", "dp"), "sp", None, None),
            P(("grp", "dp"), "sp", None),
            P(("grp", "dp"), "sp", None),
            P(),
            P("dp", "sp"),
            P(None, "dp"),
        ),
        out_specs=P(("grp", "dp"), "sp", None),
        check_vma=False,
    )
```

```python
import functools
import math

import jax
import jax.numpy as jnp
import numpy as np
from jax import lax
from jax.experimental import pallas as pl
from jax.experimental.pallas import tpu as pltpu
from jax.sharding import PartitionSpec as P

NOPE = 128
VD = 128
MESH = pl.DeviceIdType.MESH
F32 = jnp.float32
BF16 = jnp.bfloat16
FWD, BWD = 0, 1
LCH = 4
OCH = 8
WSTART = 6
WPRE = 5
XPRE = 16
NEG = -1e30


def kernel(
    nz, ndp,
    q_hbm, lat_hbm, rope_hbm, gain_hbm, wkv_hbm, wout_hbm, cos_hbm, sin_hbm,
    out_hbm,
    lbuf, rbuf, wkv, wout, qraw, qbuf, krot, kbuf, vbuf, sbuf, peak, att, obuf,
    lat, rope, gain, cosv, sinv,
    load_sem, zl_recv, zw_recv, x_recv, xw_recv, dw_recv, do_recv,
    zl_send, zd_send, zw_send, zw8_send, x_send, x4_send, xw_send, dw_send, do_send,
    out_sem, up_ready, wrap_ready, first_in,
):
    nx = ndp // 2
    hz, hx = nz // 2, nx // 2
    tok = lat.shape[0]
    kl = lat.shape[1]
    z = lax.axis_index("sp")
    dp = lax.axis_index("dp")
    x = dp // 2
    c = dp % 2
    o = 1 - c
    zdev = [{"sp": (z + 1) % nz}, {"sp": (z + nz - 1) % nz}]
    xdev = [{"dp": (dp + 2) % ndp}, {"dp": (dp + ndp - 2) % ndp}]
    mate = {"dp": x * 2 + o}

    def xsrc(d, s):
        return (x + nx - s) % nx if d == FWD else (x + s) % nx

    loads = [
        pltpu.make_async_copy(lat_hbm.at[0], lat, load_sem.at[0]),
        pltpu.make_async_copy(gain_hbm, gain, load_sem.at[1]),
        pltpu.make_async_copy(rope_hbm.at[0], rope, load_sem.at[2]),
        pltpu.make_async_copy(cos_hbm.at[z], cosv, load_sem.at[3]),
        pltpu.make_async_copy(sin_hbm.at[z], sinv, load_sem.at[4]),
        pltpu.make_async_copy(wkv_hbm, wkv.at[z, x, c], load_sem.at[5]),
        pltpu.make_async_copy(wout_hbm, wout.at[c, x], load_sem.at[6]),
        pltpu.make_async_copy(q_hbm.at[0], qraw, load_sem.at[7]),
    ]
    for copy in loads:
        copy.start()

    def clear(b, carry):
        lbuf[b] = jnp.zeros(lbuf.shape[1:], BF16)
        krot[b] = jnp.zeros(krot.shape[1:], BF16)
        return carry

    lax.fori_loop(1, nz, clear, 0)

    barrier = pltpu.get_barrier_semaphore()

    def tell(sem, peer):
        pl.semaphore_signal(sem, inc=1, device_id=peer, device_id_type=MESH)

    for peer in [mate] + [{"dp": (dp + 2 * k) % ndp} for k in range(1, nx)]:
        tell(barrier, peer)
    pl.when(z < nz - 1)(lambda: tell(barrier, zdev[FWD]))
    pl.when(z == 0)(lambda: tell(barrier, zdev[BWD]))

    for copy in loads[:5]:
        copy.wait()
    value = lat[...].astype(F32)
    norm = value * lax.rsqrt(jnp.mean(value * value, axis=-1, keepdims=True) + 1e-06)
    lbuf[0] = (norm * gain[...]).astype(BF16)
    half = rope.shape[0] // 2

    def rotated(first, second):
        first = first.astype(F32)
        second = second.astype(F32)
        cosine, sine = cosv[...], sinv[...]
        return first * cosine - second * sine, first * sine + second * cosine

    turned = rotated(rope[0:half, :], rope[half:, :])
    rbuf[0, 0:half, :] = turned[0].astype(BF16)
    rbuf[0, half:, :] = turned[1].astype(BF16)
    loads[5].wait()
    loads[6].wait()
    pl.semaphore_wait(barrier, nx + jnp.where(z > 0, 1, 0) + jnp.where(z == nz - 1, 1, 0))
    pl.when(z > 0)(lambda: tell(up_ready, zdev[BWD]))
    pl.when(z == nz - 1)(lambda: tell(wrap_ready, zdev[FWD]))

    rows = tok // LCH
    xs = nx // LCH
    orow = wout.shape[2] // OCH

    def slot(d, s):
        return s if d == FWD else (nz - s) % nz

    def all_of(ref, send_sem, recv_sem):
        return pltpu.make_async_remote_copy(
            src_ref=ref, dst_ref=ref, send_sem=send_sem, recv_sem=recv_sem,
            device_id=mate, device_id_type=MESH)

    def l_ref(b, ch):
        return rbuf.at[b] if ch == LCH else lbuf.at[b, pl.ds(ch * rows, rows)]

    def l_copy(d, s, ch):
        return pltpu.make_async_remote_copy(
            src_ref=l_ref(slot(d, s - 1), ch), dst_ref=l_ref(slot(d, s), ch),
            send_sem=zl_send.at[d, s - 1, ch], recv_sem=zl_recv.at[d, s - 1, ch],
            device_id=zdev[d], device_id_type=MESH)

    def furthest(d, ch):
        low = ch == LCH or ch < LCH // 2
        return hz if low == (d == FWD) else hz - 1

    def l_got(d, s, ch):
        if d == FWD:
            return z >= s
        return (z + s >= nz) | (z + s <= furthest(d, ch) - 1)

    def l_sent(d, s, ch):
        if d == FWD:
            return (z < nz - 1) & (z >= s - 1)
        return (z == 0) | (z + s - 1 >= nz) | (z + s - 1 <= furthest(d, ch) - 1)

    def l_event(s, ch):
        for d in (FWD, BWD):
            if s > furthest(d, ch):
                continue

            def body(d=d):
                l_copy(d, s, ch).wait_recv()
                if s + 1 <= furthest(d, ch):
                    pl.when(z < nz - 1 if d == FWD else z > 0)(l_copy(d, s + 1, ch).start)

            pl.when(l_got(d, s, ch))(body)

    def w_ref(h, ch, core):
        return wkv.at[h, pl.ds(ch * xs, xs), core]

    def w_copy(d, s, ch, h, ssem, device=None):
        return pltpu.make_async_remote_copy(
            src_ref=w_ref(h, ch, c), dst_ref=w_ref(h, ch, c), send_sem=ssem,
            recv_sem=zw_recv.at[d, s - 1, ch], device_id=zdev[d] if device is None else device,
            device_id_type=MESH)

    def w_mate(h, ch):
        return pltpu.make_async_remote_copy(
            src_ref=w_ref(h, ch, c), dst_ref=w_ref(h, ch, c), send_sem=dw_send,
            recv_sem=dw_recv.at[h], device_id=mate, device_id_type=MESH)

    nwe = LCH * (hz - 1) + LCH // 2

    def forward_distance(k):
        return jnp.where(k < z, k + 1, hz - 1 - (k - z))

    def w_event(n):
        n = jnp.int32(n)
        k = n // LCH
        j = n % LCH
        final = k == hz - 1
        for d in (FWD, BWD):
            s = jnp.where(final, hz, forward_distance(k)) if d == FWD else k + 1
            h = lax.rem(z + nz - s if d == FWD else z + s, nz)
            ch = j if d == FWD else jnp.where(final, j + LCH // 2, j)
            half_ok = (j < LCH // 2) if d == FWD else (j >= LCH // 2)
            may = z < nz - 1 if d == FWD else z >= 0
            w_copy(d, s, ch, h, zw_send.at[d]).wait_recv()
            pl.when(may & (s < hz - 1))(w_copy(d, s + 1, ch, h, zw_send.at[d]).start)
            pl.when(may & (s == hz - 1) & half_ok)(w_copy(d, s + 1, ch, h, zw8_send.at[d]).start)
            w_mate(h, ch).start()

    def o_ref(b, ch):
        return wout.at[c, b, pl.ds(ch * orow, orow)]

    def o_copy(d, s, ch, b, last):
        return pltpu.make_async_remote_copy(
            src_ref=o_ref(b, ch), dst_ref=o_ref(b, ch),
            send_sem=x4_send.at[d] if last else x_send.at[d],
            recv_sem=x_recv.at[d, s - 1, ch], device_id=xdev[d], device_id_type=MESH)

    def o_mate(b, ch):
        return pltpu.make_async_remote_copy(
            src_ref=o_ref(b, ch), dst_ref=o_ref(b, ch), send_sem=do_send,
            recv_sem=do_recv, device_id=mate, device_id_type=MESH)

    nev = OCH * (hx - 1) + OCH // 2

    def o_event(n):
        s = n // OCH + 1
        k = n % OCH
        for d in (FWD, BWD):
            b = xsrc(d, s)
            if isinstance(n, int):
                ch = k if s < hx else k + d * (OCH // 2)
                o_copy(d, s, ch, b, False).wait_recv()
                if s < hx - 1:
                    o_copy(d, s + 1, ch, b, False).start()
                elif s == hx - 1 and (k < OCH // 2) == (d == FWD):
                    o_copy(d, s + 1, ch, b, True).start()
                o_mate(b, ch).start()
            else:
                ch = jnp.where(s < hx, k, k + d * (OCH // 2))
                o_copy(d, s, ch, b, False).wait_recv()
                half_ok = (k < OCH // 2) if d == FWD else (k >= OCH // 2)

                def forward(d=d, s=s, ch=ch, b=b, last=False):
                    o_copy(d, s + 1, ch, b, last).start()

                pl.when(s < hx - 1)(forward)
                pl.when((s == hx - 1) & half_ok)(functools.partial(forward, last=True))
                o_mate(b, ch).start()

    for k in range(1, nx):
        pltpu.make_async_remote_copy(
            src_ref=wkv.at[z, x, c], dst_ref=wkv.at[z, x, c], send_sem=xw_send,
            recv_sem=xw_recv, device_id={"dp": (dp + 2 * k) % ndp}, device_id_type=MESH).start()
    for ch in range(LCH + 1):
        pl.when((z > 0) & (z <= furthest(BWD, ch) - 1))(l_copy(BWD, 1, ch).start)
    for ch in range(OCH):
        for d in (FWD, BWD):
            o_copy(d, 1, ch, x, False).start()
    for ch in range(OCH):
        o_mate(x, ch).start()

    def up_first():
        pl.semaphore_wait(up_ready, 1)
        for ch in range(LCH + 1):
            l_copy(FWD, 1, ch).start()

    pl.when(z < nz - 1)(up_first)
    loads[7].wait()

    def prepare_query(h):
        content = qraw[h, 0:NOPE, :].astype(F32)
        t0, t1 = rotated(qraw[h, NOPE:NOPE + half, :], qraw[h, NOPE + half:, :])
        pad = jnp.zeros((256 - NOPE - 2 * half, tok), F32)
        whole = jnp.concatenate([content, t0, t1, pad], axis=0)
        qbuf[h] = whole.T.astype(BF16)

    def prepare_key(b):
        key = rbuf[b].astype(F32)
        pad = jnp.zeros((128 - 2 * half, tok), F32)
        krot[b] = jnp.concatenate([key, pad], axis=0).T.astype(BF16)

    prepare_key(0)
    per = nz // hz
    done = 0
    for s in range(1, hz + 1):
        for ch in range(LCH + 1):
            l_event(s, ch)
            if ch % 2 == 1 and done < XPRE and s > 1:
                o_event(done)
                done += 1
        for d in (FWD, BWD) if s < hz else (FWD,):
            pl.when(z >= slot(d, s))(functools.partial(prepare_key, slot(d, s)))
        for j in range(per):
            prepare_query((s - 1) * per + j)
        if s == 2:
            all_of(wkv.at[z, pl.ds(0, nx - 1), c], xw_send, xw_recv).wait_recv()
            pl.when(z > 1)(lambda: pl.semaphore_wait(first_in, 1))
            pl.when((z > 0) & (z < nz - 1))(lambda: tell(first_in, zdev[FWD]))
            for ch in range(LCH):
                pl.when(z >= hz if ch < LCH // 2 else z > hz)(
                    w_copy(FWD, nz - z, ch, z, zd_send.at[ch], {"sp": 0}).start)
                pl.when(z > 0)(w_copy(BWD, 1, ch, z, zw_send.at[BWD]).start)
                pl.when(z < hz)(w_copy(FWD, 1, ch, z, zw_send.at[FWD]).start)
            for ch in range(LCH):
                w_mate(z, ch).start()
        if s == WSTART:
            for ch in range(LCH):
                pl.when((z >= hz) & (z < nz - 1))(w_copy(FWD, 1, ch, z, zw_send.at[FWD]).start)

    def round_the_wrap():
        pl.semaphore_wait(wrap_ready, 1)
        for s in range(1, hz + 1):
            for ch in range(LCH + 1):
                if s <= furthest(BWD, ch):
                    l_copy(BWD, s, ch).start()
        for ch in range(LCH):
            w_copy(BWD, 1, ch, z, zw_send.at[BWD]).start()

    pl.when(z == 0)(round_the_wrap)
    while done < XPRE:
        o_event(done)
        done += 1

    span = 4 * tok
    parts = nz // 4
    scale = float((2 * half + NOPE) ** -0.5 * math.log2(math.e))

    bias = [None] + [jnp.where(z >= j, 0.0, NEG).astype(F32) for j in range(1, nz)]
    sizes = [(z < 4, 1), ((z >= 4) & (z < 8), 2), (z >= 8, parts)]

    def up_project(h, par, t):
        weights = wkv[h].reshape(kl, NOPE + VD)
        block = lbuf[4 * t:4 * t + 4].reshape(span, kl)
        kv = jnp.dot(block, weights, preferred_element_type=F32).astype(BF16)
        kbuf[par, 4 * t:4 * t + 4] = kv[:, :NOPE].reshape(4, tok, NOPE)
        vbuf[par, 4 * t:4 * t + 4] = kv[:, NOPE:].reshape(4, tok, VD)

    def head_of(i):
        k = i // 2
        ahead = jnp.where(i == nz - 1, hz, jnp.where(i % 2 == 1, nz - forward_distance(k), k))
        return lax.rem(z + ahead, nz)

    def find_scores(h, par, tiles):
        query = qbuf[h]
        top = jnp.full((tok, 128), NEG, F32)
        for t in range(tiles):
            keys = jnp.concatenate(
                [kbuf[par, 4 * t:4 * t + 4].reshape(span, NOPE),
                 krot[4 * t:4 * t + 4].reshape(span, 128)], axis=1)
            sc = lax.dot_general(query, keys, (((1,), (1,)), ((), ())), preferred_element_type=F32)
            for j in range(4):
                piece = sc[:, j * tok:(j + 1) * tok] * scale
                if t == 0 and j == 0:
                    row = lax.broadcasted_iota(jnp.int32, (tok, tok), 0)
                    col = lax.broadcasted_iota(jnp.int32, (tok, tok), 1)
                    piece = jnp.where(col <= row, piece, NEG)
                else:
                    piece = piece + bias[4 * t + j]
                sbuf[:, (4 * t + j) * tok:(4 * t + j + 1) * tok] = piece
                top = jnp.maximum(top, piece)
        peak[...] = jnp.broadcast_to(jnp.max(top, axis=-1, keepdims=True), (tok, 128))

    def attend(h, par, tiles, following):
        high = jnp.max(peak[...], axis=-1, keepdims=True)
        total = jnp.zeros((tok, 128), F32)
        result = jnp.zeros((tok, VD), F32)
        for t in range(tiles):
            expo = jnp.exp2(sbuf[:, t * span:(t + 1) * span] - high)
            for j in range(span // 128):
                total = total + expo[:, j * 128:(j + 1) * 128]
            vals = vbuf[par, 4 * t:4 * t + 4].reshape(span, VD)
            result = result + jnp.dot(expo.astype(BF16), vals, preferred_element_type=F32)
            if following is not None:
                up_project(following, 1 - par, t)
        denom = jnp.sum(total, axis=-1, keepdims=True)
        att[h] = (result / denom).astype(BF16)

    for n in range(WPRE):
        w_event(n)
    all_of(wkv.at[z, :, o], dw_send, dw_recv.at[z]).wait_recv()
    for t in range(parts):
        pl.when(z >= min(4 * t, 8))(functools.partial(up_project, z, 0, t))

    def one_head(i, carry):
        par = lax.rem(i, 2)
        h, following = head_of(i), head_of(i + 1)
        for cond, tiles in sizes:
            pl.when(cond)(functools.partial(find_scores, h, par, tiles))
        pl.when(2 * i + WPRE < nwe)(lambda: w_event(2 * i + WPRE))
        pl.when(i < nev - XPRE)(lambda: o_event(i + XPRE))
        all_of(wkv.at[following, :, o], dw_send, dw_recv.at[following]).wait_recv()
        for cond, tiles in sizes:
            pl.when(cond)(functools.partial(attend, h, par, tiles, following))
        pl.when(2 * i + WPRE + 1 < nwe)(lambda: w_event(2 * i + WPRE + 1))
        return carry

    lax.fori_loop(0, nz - 1, one_head, 0)
    last_head = head_of(jnp.int32(nz - 1))
    for cond, tiles in sizes:
        pl.when(cond)(functools.partial(find_scores, last_head, (nz - 1) % 2, tiles))
        pl.when(cond)(functools.partial(attend, last_head, (nz - 1) % 2, tiles, None))

    all_of(wout.at[o], do_send, do_recv).wait_recv()
    attended = jnp.concatenate([att[h] for h in range(nz)], axis=1)

    def out_copy(b):
        return pltpu.make_async_copy(
            obuf.at[b], out_hbm.at[0, :, pl.ds(b * 256, 256)], out_sem.at[b])

    def project(b, carry):
        cols = jnp.concatenate([wout[0, b], wout[1, b]], axis=1)
        obuf[b] = jnp.dot(attended, cols, preferred_element_type=F32).astype(BF16)
        out_copy(b).start()
        return carry

    lax.fori_loop(0, nx, project, 0)

    all_of(wkv.at[0, pl.ds(0, nx - 1), 0], xw_send, xw_recv).wait_send()
    for s in range(1, hz + 1):
        for ch in range(LCH + 1):
            for d in (FWD, BWD):
                if s <= furthest(d, ch):
                    pl.when(l_sent(d, s, ch))(l_copy(d, s, ch).wait_send)
    for ch in range(LCH):
        pl.when(z >= hz if ch < LCH // 2 else z > hz)(
            w_copy(FWD, 1, ch, z, zd_send.at[ch]).wait_send)
    for d in (FWD, BWD):

        def weights_sent(d=d):
            all_of(wkv.at[pl.ds(0, hz - 1), :, 0], zw_send.at[d], xw_recv).wait_send()
            all_of(wkv.at[0, pl.ds(0, nx // 2), 0], zw8_send.at[d], xw_recv).wait_send()

        pl.when(z < nz - 1 if d == FWD else z >= 0)(weights_sent)
        all_of(wout.at[0, pl.ds(0, hx - 1)], x_send.at[d], xw_recv).wait_send()
        all_of(wout.at[0, 0, pl.ds(0, wout.shape[2] // 2)], x4_send.at[d], xw_recv).wait_send()
    all_of(wkv.at[:, :, 0], dw_send, xw_recv).wait_send()
    all_of(wout.at[0], do_send, xw_recv).wait_send()
    for b in range(nx):
        out_copy(b).wait()


def body(nz, ndp, queries, kv_latent, rope_key, kv_gain, kv_weight, out_weight):
    tok, heads, width = queries.shape[1:]
    kl = kv_latent.shape[2]
    rot = rope_key.shape[2]
    half = rot // 2
    nx = ndp // 2
    hz, hx = nz // 2, nx // 2
    model = out_weight.shape[1] * ndp
    pos = np.arange(nz * tok, dtype=np.float32)
    inverse = np.power(np.float32(10000.0), -np.arange(half, dtype=np.float32) * np.float32(2.0) / np.float32(rot))
    angle = (pos[:, None] * inverse.astype(np.float32)).astype(np.float32).astype(np.float64)
    table = lambda f: jnp.asarray(
        f(angle).astype(np.float32).reshape(nz, tok, half).transpose(0, 2, 1))
    dma = pltpu.SemaphoreType.DMA
    anyspec = pl.BlockSpec(memory_space=pl.ANY)
    call = pl.pallas_call(
        functools.partial(kernel, nz, ndp),
        out_shape=jax.ShapeDtypeStruct((1, tok, model), BF16),
        in_specs=[anyspec] * 8,
        out_specs=anyspec,
        scratch_shapes=[
            pltpu.VMEM((nz, tok, kl), BF16),
            pltpu.VMEM((nz, rot, tok), BF16),
            pltpu.VMEM((nz, nx, 2, kl // ndp, NOPE + VD), BF16),
            pltpu.VMEM((2, nx, heads * VD, model // ndp), BF16),
            pltpu.VMEM((heads, width, tok), BF16),
            pltpu.VMEM((heads, tok, 256), BF16),
            pltpu.VMEM((nz, tok, 128), BF16),
            pltpu.VMEM((2, nz, tok, NOPE), BF16),
            pltpu.VMEM((2, nz, tok, VD), BF16),
            pltpu.VMEM((tok, nz * tok), F32),
            pltpu.VMEM((tok, 128), F32),
            pltpu.VMEM((heads, tok, VD), BF16),
            pltpu.VMEM((nx, tok, 256), BF16),
            pltpu.VMEM((tok, kl), BF16),
            pltpu.VMEM((rot, tok), BF16),
            pltpu.VMEM((1, kl), F32),
            pltpu.VMEM((half, tok), F32),
            pltpu.VMEM((half, tok), F32),
            dma((8,)),
            dma((2, hz, LCH + 1)),
            dma((2, hz, LCH)),
            dma((2, hx, OCH)),
            dma, dma((nz,)), dma,
            dma((2, hz, LCH + 1)), dma((LCH,)), dma((2,)), dma((2,)), dma((2,)), dma((2,)),
            dma, dma, dma,
            dma((nx,)),
            pltpu.SemaphoreType.REGULAR, pltpu.SemaphoreType.REGULAR, pltpu.SemaphoreType.REGULAR,
        ],
        compiler_params=pltpu.CompilerParams(
            collective_id=0, has_side_effects=True, vmem_limit_bytes=60 * 1024 * 1024),
    )
    return call(
        jnp.transpose(queries, (0, 2, 3, 1)), kv_latent, jnp.transpose(rope_key, (0, 2, 1)),
        kv_gain.reshape(1, kl), kv_weight, out_weight, table(np.cos), table(np.sin))


def solution(mesh):
    return jax.shard_map(
        functools.partial(body, mesh.shape["sp"], mesh.shape["dp"]),
        mesh=mesh,
        in_specs=(
            P(("grp", "dp"), "sp", None, None),
            P(("grp", "dp"), "sp", None),
            P(("grp", "dp"), "sp", None),
            P(),
            P("dp", "sp"),
            P(None, "dp"),
        ),
        out_specs=P(("grp", "dp"), "sp", None),
        check_vma=False,
    )
```
